32 devices in a mesh: sp: 8 (over z, x), tp: 4 (over y, core).
Axes of the slice: x: 2, y: 2, z: 4, core: 2. Of those that a mesh axis runs over, the one named last changes fastest.
Arguments:
- tokens: bfloat16 [1536, 2048], P(('sp', 'tp')), may hold values from -7 to 7
- input_norm_gain: float32 [2048], replicated, may hold values from 0.1 to 1.9
- paired_query_weight: bfloat16 [2048, 512], P('sp', 'tp'), may hold values from -16 to 16
- shared_key_weight: bfloat16 [2048, 64], replicated, may hold values from -1 to 1
- shared_value_weight: bfloat16 [2048, 64], replicated, may hold values from -0.125 to 0.125
- recurrent_query_weight: bfloat16 [2048, 1024], P('sp', 'tp'), may hold values from -0.125 to 0.125
- forget_gate_weight: bfloat16 [2048, 1024], P('sp', 'tp'), may hold values from -0.125 to 0.125
- recurrent_value_weight: bfloat16 [2048, 1024], P('sp', 'tp'), may hold values from -0.125 to 0.125
- attention_output_weight: bfloat16 [2048, 512], P('sp', 'tp'), may hold values from -0.15625 to 0.15625
- recurrent_output_weight: bfloat16 [2048, 1024], P('sp', 'tp'), may hold values from -0.15625 to 0.15625
- attention_head_gain: float32 [64], replicated, may hold values from 0.1 to 1.9
- recurrent_head_gain: float32 [128], replicated, may hold values from 0.1 to 1.9
- second_map_weight: float32 [8], P('tp'), may hold values from 0.3 to 0.8
- forget_leak_rate: float32 [1024], P('tp'), may hold values from 2e-05 to 0.05
- extra_log_decay: float32 [1536, 1024], P('sp', 'tp'), may hold values from -1 to 0
- initial_recurrent_state: float32 [8, 128, 128], P('tp'), may hold values from -0.12 to 0.12
Outputs:
- mixer_out: bfloat16 [1536, 2048], P(('sp', 'tp'))
The draws below stay inside these ranges and needn't reach their ends.
All inputs are finite; a program needn't handle non-finite values.
Results may differ from the reference program's by a relative error of at most 0.014.
Values may be sent and summed in bfloat16 or wider, within the bound.
A program may use at most 128 MiB of HBM per device.

```python
import math
import jax
import jax.numpy as jnp
from jax import lax

D = 2048
DIFF_HEADS = 8
QK_DIM = 32
HEAD_DIM = 64
RECURRENT_HEADS = 8
RECURRENT_WIDTH = 128
REC_SPAN = 64
TOKEN_COUNT = 1536
N_TP = 4


def pair_raw(key):
    key_raw = jnp.clip(jax.random.normal(jax.random.fold_in(key, 101), (D, 2 * QK_DIM), jnp.float32), -4.0, 4.0)
    query_raw = jnp.clip(jax.random.normal(jax.random.fold_in(key, 102), (D, DIFF_HEADS * 2 * QK_DIM), jnp.float32), -4.0, 4.0)
    return (key_raw, query_raw)


def draw_shared_key_weight(key, part):
    key_raw, query_raw = pair_raw(key)
    return (key_raw * (2.0 / D) ** 0.5).astype(jnp.bfloat16)


def draw_paired_query_weight(key, part):
    key_raw, query_raw = pair_raw(key)
    weight_scale = (2.0 / D) ** 0.5
    return (query_raw * weight_scale).astype(jnp.bfloat16)


def draw_tokens(key, part):
    base_rows = jnp.clip(jax.random.normal(jax.random.fold_in(key, 201), (TOKEN_COUNT, D), jnp.float32), -6.0, 6.0)
    return base_rows.astype(jnp.bfloat16)


def draw_extra_log_decay(key, part):
    extra_decay_positions = jax.random.randint(jax.random.fold_in(key, 301), (8, RECURRENT_HEADS), 0, TOKEN_COUNT)
    row_position_index = jnp.arange(TOKEN_COUNT)
    extra_decay_flag = jnp.any(row_position_index[:, None, None] == extra_decay_positions[None], axis=1)
    extra_decay_depth = jax.random.uniform(jax.random.fold_in(key, 302), (TOKEN_COUNT, RECURRENT_HEADS), jnp.float32, jnp.log(0.5), jnp.log(0.8))
    extra_decay_field = jnp.where(extra_decay_flag, extra_decay_depth, 0.0)
    return jnp.repeat(extra_decay_field, RECURRENT_WIDTH, axis=1).astype(jnp.float32)


def block_scale(stream_key, extent, cuts, smallest, largest):
    factor_of, own = 1.0, jax.random.fold_in(stream_key, 6)
    for position, parts in cuts:
        heights = jnp.exp(jax.random.uniform(jax.random.fold_in(own, position), (parts,), jnp.float32, smallest / len(cuts), largest / len(cuts)))
        factor_of = factor_of * jnp.repeat(heights, extent[position] // parts).reshape([-1 if axis == position else 1 for axis in range(len(extent))])
    return factor_of


def centred(key, shape, deviation, reach, split=(), held_as=jnp.bfloat16):
    values = jax.random.normal(key, shape, jnp.float32) * deviation
    if len(split) > 0:
        values = block_scale(key, shape, split, -0.22, 0.18) * values
    return jnp.clip(values, min=-reach, max=reach).astype(held_as)


def setup_inputs(seed: int = 0) -> dict:
    seeds = jax.random.split(jax.random.key(seed), 17)
    return {
        "tokens": draw_tokens(jax.random.fold_in(seeds[16], 71), 0),
        "input_norm_gain": jnp.clip(1.0 + 0.18 * jax.random.normal(seeds[1], (D,), jnp.float32), 0.1, 1.9),
        "paired_query_weight": draw_paired_query_weight(jax.random.fold_in(seeds[16], 71), 0),
        "shared_key_weight": draw_shared_key_weight(jax.random.fold_in(seeds[16], 71), 0),
        "shared_value_weight": centred(seeds[4], (D, HEAD_DIM), D ** -0.5, 0.125),
        "recurrent_query_weight": centred(seeds[5], (D, RECURRENT_HEADS * RECURRENT_WIDTH), D ** -0.5, 0.125, ((0, 8), (1, 4))),
        "forget_gate_weight": centred(seeds[6], (D, RECURRENT_HEADS * RECURRENT_WIDTH), D ** -0.5, 0.125, ((0, 8), (1, 4))),
        "recurrent_value_weight": centred(seeds[7], (D, RECURRENT_HEADS * RECURRENT_WIDTH), D ** -0.5, 0.125, ((0, 8), (1, 4))),
        "attention_output_weight": centred(seeds[8], (D, DIFF_HEADS * HEAD_DIM), (DIFF_HEADS * HEAD_DIM + RECURRENT_HEADS * RECURRENT_WIDTH) ** -0.5, 0.15625, ((0, 8), (1, 4))),
        "recurrent_output_weight": centred(seeds[9], (D, RECURRENT_HEADS * RECURRENT_WIDTH), (DIFF_HEADS * HEAD_DIM + RECURRENT_HEADS * RECURRENT_WIDTH) ** -0.5, 0.15625, ((0, 8), (1, 4))),
        "attention_head_gain": jnp.clip(1.0 + 0.18 * jax.random.normal(seeds[10], (HEAD_DIM,), jnp.float32), 0.1, 1.9),
        "recurrent_head_gain": jnp.clip(1.0 + 0.18 * jax.random.normal(seeds[11], (RECURRENT_WIDTH,), jnp.float32), 0.1, 1.9),
        "second_map_weight": jnp.clip(0.3 + 0.5 * jax.random.uniform(seeds[12], (DIFF_HEADS,), jnp.float32) ** block_scale(seeds[12], (DIFF_HEADS,), ((0, 4),), -0.2, 0.2), 0.3, 0.8),
        "forget_leak_rate": jnp.clip(jnp.exp(math.log(0.05) - 7.824046 * jax.random.uniform(seeds[13], (RECURRENT_HEADS * RECURRENT_WIDTH,), jnp.float32) ** block_scale(seeds[13], (RECURRENT_HEADS * RECURRENT_WIDTH,), ((0, 4),), -0.2, 0.2)), 1.9999999494757503e-05, 0.05),
        "extra_log_decay": draw_extra_log_decay(jax.random.fold_in(seeds[16], 71), 0),
        "initial_recurrent_state": centred(seeds[15], (RECURRENT_HEADS, RECURRENT_WIDTH, RECURRENT_WIDTH), 0.02, 0.12, ((0, 4),), jnp.float32),
    }


epsilon = 1e-06

def rms_scale(matrix, gain):
    return matrix * lax.rsqrt(lax.optimization_barrier(jnp.mean(matrix * matrix, axis=-1, keepdims=True)) + epsilon) * gain

def project(normed, weight):
    return jnp.dot(normed, weight, preferred_element_type=jnp.float32).astype(jnp.bfloat16)

def widen(stored):
    return lax.optimization_barrier(stored).astype(jnp.float32)

def attend(queries, keys, values, second_map_weight, attention_head_gain):
    token_count = queries.shape[0]
    block_rows = math.gcd(token_count, 512)
    head_count = queries.shape[1] // (2 * QK_DIM)
    key_pair = keys.reshape(token_count, 2, QK_DIM)
    score_scale = 1.0 / math.sqrt(QK_DIM)

    def one_block(begin_row):
        query_rows = lax.dynamic_slice_in_dim(queries, begin_row, block_rows, 0).reshape(block_rows, head_count, 2, QK_DIM)
        head_outs = []
        for head_index in range(head_count):
            parts_list = []
            for component in range(2):
                scores = jnp.dot(query_rows[:, head_index, component], key_pair[:, component].T, preferred_element_type=jnp.float32) * score_scale
                peak_score = lax.optimization_barrier(jnp.max(scores, axis=1, keepdims=True))
                expo_terms = jnp.exp(scores - peak_score)
                totals = lax.optimization_barrier(jnp.sum(expo_terms, axis=1, keepdims=True))
                weighted = jnp.dot(expo_terms.astype(jnp.bfloat16), values, preferred_element_type=jnp.float32)
                parts_list.append(weighted / totals)
            blended = parts_list[0] - second_map_weight[head_index] * parts_list[1]
            head_outs.append(rms_scale(blended, attention_head_gain))
        return jnp.concatenate(head_outs, axis=1).astype(jnp.bfloat16)
    starts = jnp.arange(token_count // block_rows, dtype=jnp.int32) * block_rows
    pieces = lax.map(one_block, starts)
    return pieces.reshape(token_count, head_count * HEAD_DIM)

def recur_blocks(rec_query, inflow_state, rec_values, log_decay_values, initial):
    head_count, token_count, channel_width = rec_query.shape
    span_count = token_count // REC_SPAN

    def to_spans(matrix):
        return jnp.moveaxis(matrix.reshape(head_count, span_count, REC_SPAN, matrix.shape[-1]), 1, 0)
    lower_mask = jnp.tril(jnp.ones((REC_SPAN, REC_SPAN), jnp.float32))
    highest_precision = lax.Precision.HIGHEST

    def step(carried_state, inputs):
        query_span, inflow_span, value_segment, decay_span = inputs
        running = jnp.cumsum(decay_span, axis=1)
        segment_final = running[:, -1:, :]
        decayed_query = query_span * jnp.exp(running)
        inflow_dec = inflow_span * jnp.exp(-running)
        within_segment = jnp.einsum('hsk,htk->hst', decayed_query, inflow_dec, precision=highest_precision) * lower_mask
        segment_output = jnp.einsum('rcn,rni->rci', within_segment, value_segment, precision=highest_precision) + jnp.einsum('cwi,cip->cwp', decayed_query, carried_state, precision=highest_precision)
        inflow_final = inflow_span * jnp.exp(segment_final - running)
        carried_state = jnp.exp(segment_final)[:, 0, :, None] * carried_state + jnp.einsum('rgc,rgt->rct', inflow_final, value_segment, precision=highest_precision)
        return (carried_state, segment_output)
    final_state, span_outs = lax.scan(step, initial, (to_spans(rec_query), to_spans(inflow_state), to_spans(rec_values), to_spans(log_decay_values)))
    return jnp.moveaxis(span_outs, 0, 1).reshape(head_count, token_count, rec_values.shape[-1])

def reference(tokens, input_norm_gain, paired_query_weight, shared_key_weight, shared_value_weight, recurrent_query_weight, forget_gate_weight, recurrent_value_weight, attention_output_weight, recurrent_output_weight, attention_head_gain, recurrent_head_gain, second_map_weight, forget_leak_rate, extra_log_decay, initial_recurrent_state):
    token_count = tokens.shape[0]
    normed = rms_scale(tokens.astype(jnp.float32), input_norm_gain).astype(jnp.bfloat16)
    queries = project(normed, paired_query_weight)
    keys = project(normed, shared_key_weight)
    values = project(normed, shared_value_weight)
    attn_hidden = attend(queries, keys, values, second_map_weight, attention_head_gain)
    rec_query = jax.nn.silu(widen(project(normed, recurrent_query_weight)))
    gate_raw = widen(project(normed, forget_gate_weight))
    rec_values = widen(project(normed, recurrent_value_weight))
    inflow_state = forget_leak_rate * (1.0 - jax.nn.sigmoid(gate_raw))
    log_decay_values = jnp.log(1.0 - inflow_state) + extra_log_decay

    def heads_first(matrix):
        return matrix.reshape(token_count, RECURRENT_HEADS, RECURRENT_WIDTH).transpose(1, 0, 2)
    recurrent_output = recur_blocks(heads_first(rec_query), heads_first(inflow_state), heads_first(rec_values), heads_first(log_decay_values), initial_recurrent_state)
    rec_hidden = rms_scale(recurrent_output, recurrent_head_gain).transpose(1, 0, 2).reshape(token_count, RECURRENT_HEADS * RECURRENT_WIDTH)
    rec_hidden = rec_hidden.astype(jnp.bfloat16)
    attn_group = DIFF_HEADS * HEAD_DIM // N_TP
    rec_group = RECURRENT_HEADS * RECURRENT_WIDTH // N_TP
    summed = jnp.zeros((token_count, D), jnp.float32)
    for group_index in range(N_TP):
        attn_cols = slice(group_index * attn_group, (group_index + 1) * attn_group)
        rec_cols = slice(group_index * rec_group, (group_index + 1) * rec_group)
        group_part = jnp.dot(attn_hidden[:, attn_cols], attention_output_weight[:, attn_cols].T, preferred_element_type=jnp.float32) + jnp.dot(rec_hidden[:, rec_cols], recurrent_output_weight[:, rec_cols].T, preferred_element_type=jnp.float32)
        summed = summed + lax.optimization_barrier(group_part.astype(jnp.bfloat16)).astype(jnp.float32)
    return summed.astype(jnp.bfloat16)
```

```python
import functools
import math

import jax
import jax.numpy as jnp
from jax import lax
from jax.experimental import pallas as pl
from jax.experimental.pallas import tpu as pltpu
from jax.sharding import PartitionSpec as P

QK_DIM = 32
HEAD_DIM = 64
RECURRENT_WIDTH = 128
REC_SPAN = 64
KEY_BLOCK = 1536
EPS = 1e-06
MESH = pl.DeviceIdType.MESH
F32, BF16 = jnp.float32, jnp.bfloat16

NN = (((1,), (0,)), ((), ()))
NT = (((1,), (1,)), ((), ()))
TN = (((0,), (0,)), ((), ()))


def dot(a, b, dims=NN, precision=None):
    return lax.dot_general(a, b, dims, preferred_element_type=F32, precision=precision)


def rms(x, gain):
    return x * lax.rsqrt(jnp.mean(x * x, axis=-1, keepdims=True) + EPS) * gain


def loop(lo, hi, body):
    def step(j, carry):
        body(j)
        return carry

    lax.fori_loop(lo, hi, step, 0)


def kernel(
    n, nt,
    tok, gain, wq, wg, wv, wr, woa, wor, wk, wval, again, rgain, mapw, leak, extra, init,
    out,
    gq, gg, gv, gr, goa, gor, nf, kv, state, decay, pbuf, rbuf,
    ring_send, ring_recv, n_send, n_recv, kv_send, kv_recv, kt_send, kt_recv,
    st_send, st_recv, de_send, de_recv, o_send, o_recv,
):
    s, t = lax.axis_index("sp"), lax.axis_index("tp")
    half = n // 2
    x, z = s % 2, s // 2
    pos = (1 - x) * z + x * (n - 1 - z)

    def at(p):
        p = (p + 2 * n) % n
        hi = p // half
        return (1 - hi) * 2 * p + hi * (2 * (n - 1 - p) + 1)

    ins = (wq, wg, wv, wr, woa, wor)
    bufs = (gq, gg, gv, gr, goa, gor)
    longer = (0, 0, 1, 0, 1, 1)

    def hops(a, d):
        return half if longer[a] == d else half - 1

    def send(a, d, k, first):
        sign = 1 - 2 * d
        owner = s if first else at(pos - sign * k)
        return pltpu.make_async_remote_copy(
            src_ref=ins[a] if first else bufs[a].at[owner],
            dst_ref=bufs[a].at[owner],
            send_sem=ring_send.at[a, d, k],
            recv_sem=ring_recv.at[a, d, k],
            device_id=(at(pos + sign), t),
            device_id_type=MESH,
        )

    def arrival(a, d, k):
        sign = 1 - 2 * d
        slot = bufs[a].at[at(pos - sign * (k + 1))]
        return pltpu.make_async_remote_copy(
            src_ref=slot, dst_ref=slot,
            send_sem=ring_send.at[a, d, k], recv_sem=ring_recv.at[a, d, k],
            device_id=(at(pos - sign), t), device_id_type=MESH,
        )

    def start(group):
        for a in group:
            for d in (0, 1):
                send(a, d, 0, True).start()

    def ring_hop(group, k):
        for a in group:
            for d in (0, 1):
                count = hops(a, d)

                @pl.when(k < count)
                def _():
                    arrival(a, d, k).wait_recv()

                @pl.when(k + 1 < count)
                def _():
                    send(a, d, k + 1, False).start()

    def ring(group, lo, hi):
        if n <= 8:
            for k in range(lo, hi):
                ring_hop(group, k)
        else:
            loop(lo, hi, lambda k: ring_hop(group, k))

    def finish(group):
        for a in group:
            for d in (0, 1):
                send(a, d, 0, True).wait_send()
                loop(1, hops(a, d), lambda k: send(a, d, k, False).wait_send())

    one, two = (0, 1, 2), (3, 4, 5)
    cut = [half * i // 4 for i in range(5)]
    start(one)

    rows = tok.shape[0]
    normed = rms(tok[...].astype(F32), gain[...]).astype(BF16)
    nf[t] = normed

    def tp_peer(j):
        return (t + j) % nt

    def n_copy(j):
        return pltpu.make_async_remote_copy(
            src_ref=nf.at[t], dst_ref=nf.at[t], send_sem=n_send.at[j], recv_sem=n_recv.at[j],
            device_id=(s, tp_peer(j)), device_id_type=MESH,
        )

    def n_in(j):
        slot = nf.at[(t + nt - j) % nt]
        return pltpu.make_async_remote_copy(
            src_ref=slot, dst_ref=slot, send_sem=n_send.at[j], recv_sem=n_recv.at[j],
            device_id=(s, (t + nt - j) % nt), device_id_type=MESH,
        )

    kv[t, s] = jnp.concatenate(
        [dot(normed, wk[...]).astype(BF16), dot(normed, wval[...]).astype(BF16)], axis=1
    )
    for j in range(1, nt):
        n_copy(j).start()

    def kv_copy(j):
        return pltpu.make_async_remote_copy(
            src_ref=kv.at[t, s], dst_ref=kv.at[t, s],
            send_sem=kv_send.at[j], recv_sem=kv_recv.at[j],
            device_id=((s + j) % n, t), device_id_type=MESH,
        )

    def kv_in(j):
        slot = kv.at[t, (s + n - j) % n]
        return pltpu.make_async_remote_copy(
            src_ref=slot, dst_ref=slot, send_sem=kv_send.at[j], recv_sem=kv_recv.at[j],
            device_id=((s + n - j) % n, t), device_id_type=MESH,
        )

    def kt_copy(j):
        return pltpu.make_async_remote_copy(
            src_ref=kv.at[t], dst_ref=kv.at[t], send_sem=kt_send.at[j], recv_sem=kt_recv.at[j],
            device_id=(s, tp_peer(j)), device_id_type=MESH,
        )

    def kt_in(j):
        slot = kv.at[(t + nt - j) % nt]
        return pltpu.make_async_remote_copy(
            src_ref=slot, dst_ref=slot, send_sem=kt_send.at[j], recv_sem=kt_recv.at[j],
            device_id=(s, (t + nt - j) % nt), device_id_type=MESH,
        )

    loop(1, n, lambda j: kv_copy(j).start())
    for a in range(6):
        bufs[a][s] = ins[a][...]

    ring(one, 0, max(cut[1], 1))
    loop(1, n, lambda j: kv_in(j).wait_recv())
    for j in range(1, nt):
        kt_copy(j).start()
    ring(one, max(cut[1], 1), half - 1)
    start(two)
    for j in range(1, nt):
        n_in(j).wait_recv()
        kt_in(j).wait_recv()
    ring(one, half - 1, half)

    count = nt * rows
    full = nf[...].reshape(count, nf.shape[2])

    def project(buf):
        return dot(full, buf[...].reshape(full.shape[1], buf.shape[2])).astype(BF16)

    queries = project(gq)
    gate = project(gg).astype(F32)
    vals = project(gv)
    ring(two, cut[0], cut[1])

    inflow = leak[...] * (1.0 - jax.nn.sigmoid(gate))
    log_decay = jnp.log(1.0 - inflow) + extra[...]
    spans = count // REC_SPAN
    rr = lax.broadcasted_iota(jnp.int32, (REC_SPAN, REC_SPAN), 0)
    cc = lax.broadcasted_iota(jnp.int32, (REC_SPAN, REC_SPAN), 1)
    lower = (rr >= cc).astype(F32)
    running, offsets = [], []
    offset = jnp.zeros((1, log_decay.shape[1]), F32)
    for i in range(spans):
        part = log_decay[i * REC_SPAN : (i + 1) * REC_SPAN]
        run = dot(lower, part, precision=lax.Precision.HIGHEST)
        running.append(run)
        offsets.append(offset)
        offset = offset + run[REC_SPAN - 1 : REC_SPAN]
    total = offset
    heads = log_decay.shape[1] // RECURRENT_WIDTH
    befores = [[None] * spans for _ in range(heads)]
    for h in range(heads):
        c = slice(h * RECURRENT_WIDTH, (h + 1) * RECURRENT_WIDTH)
        carried = None
        for i in range(spans):
            r = slice(i * REC_SPAN, (i + 1) * REC_SPAN)
            befores[h][i] = carried
            final = running[i][REC_SPAN - 1 : REC_SPAN, c]
            weight = (inflow[r, c] * jnp.exp(final - running[i][:, c])).astype(BF16)
            new = dot(vals[r, c], weight, TN)
            carried = new if carried is None else carried * jnp.exp(final) + new
        state[s, h] = carried.astype(BF16)
    decay[s] = jnp.broadcast_to(total, decay.shape[1:])

    def st_pair(j, peer, owner):
        return (
            pltpu.make_async_remote_copy(
                src_ref=state.at[owner], dst_ref=state.at[owner],
                send_sem=st_send.at[j], recv_sem=st_recv.at[j],
                device_id=(peer, t), device_id_type=MESH,
            ),
            pltpu.make_async_remote_copy(
                src_ref=decay.at[owner], dst_ref=decay.at[owner],
                send_sem=de_send.at[j], recv_sem=de_recv.at[j],
                device_id=(peer, t), device_id_type=MESH,
            ),
        )

    def st_start(j):
        for copy in st_pair(j, s + j, s):
            copy.start()

    def st_wait(j):
        for copy in st_pair(j, s - j, s - j):
            copy.wait_recv()

    loop(1, n - s, st_start)
    ring(two, cut[1], cut[2])

    key_total = kv.shape[0] * kv.shape[1] * kv.shape[2]
    owners = max(1, min(n, KEY_BLOCK // (nt * rows)))
    blocks = n // owners
    scale = 1.0 / math.sqrt(QK_DIM)

    def attend(h, b):
        both = kv[:, pl.ds(b * owners, owners)].reshape(nt * owners * rows, kv.shape[3])
        values = both[:, 2 * QK_DIM :]
        parts = []
        for comp in range(2):
            lo = (2 * h + comp) * QK_DIM
            keys = both[:, comp * QK_DIM : (comp + 1) * QK_DIM]
            scores = dot(queries[:, lo : lo + QK_DIM], keys, NT) * scale
            peak = jnp.max(scores, axis=1, keepdims=True)
            expo = jnp.exp(scores - peak)
            parts += [peak, jnp.sum(expo, axis=1, keepdims=True), dot(expo.astype(BF16), values)]
        return tuple(parts)

    def merge(a, b):
        parts = []
        for comp in range(2):
            pa, ta, wa = a[3 * comp : 3 * comp + 3]
            pb, tb, wb = b[3 * comp : 3 * comp + 3]
            peak = jnp.maximum(pa, pb)
            ea, eb = jnp.exp(pa - peak), jnp.exp(pb - peak)
            parts += [peak, ta * ea + tb * eb, wa * ea + wb * eb]
        return tuple(parts)

    attn_heads = queries.shape[1] // (2 * QK_DIM)
    hidden = []
    for h in range(attn_heads):
        got = attend(h, 0)
        if blocks > 1:
            got = lax.fori_loop(1, blocks, lambda b, g: merge(g, attend(h, b)), got)
        blended = got[2] / got[1] - mapw[h] * (got[5] / got[4])
        hidden.append(rms(blended, again[...]))
        if h == 0:
            ring(two, cut[2], cut[3])
    attn_hidden = jnp.concatenate(hidden, axis=1).astype(BF16)
    ring(two, cut[3], cut[4])

    raw = project(gr).astype(F32)
    rec_query = raw * jax.nn.sigmoid(raw)
    local, lifted = [], []
    for h in range(heads):
        c = slice(h * RECURRENT_WIDTH, (h + 1) * RECURRENT_WIDTH)
        outs, lifts = [], []
        for i in range(spans):
            r = slice(i * REC_SPAN, (i + 1) * REC_SPAN)
            run = running[i][:, c]
            dq = (rec_query[r, c] * jnp.exp(run)).astype(BF16)
            within = dot(dq, (inflow[r, c] * jnp.exp(-run)).astype(BF16), NT) * lower
            o = dot(within.astype(BF16), vals[r, c])
            if befores[h][i] is not None:
                o = o + dot(dq, befores[h][i].astype(BF16), NT)
            outs.append(o)
            lifts.append(rec_query[r, c] * jnp.exp(offsets[i][:, c] + run))
        local.append(jnp.concatenate(outs, axis=0))
        lifted.append(jnp.concatenate(lifts, axis=0).astype(BF16))

    loop(1, s + 1, st_wait)
    first = tuple(init[h].T for h in range(heads))

    def chain(k, carry):
        d = jnp.exp(decay[k][0:1])
        return tuple(
            carry[h] * d[:, h * RECURRENT_WIDTH : (h + 1) * RECURRENT_WIDTH]
            + state[k, h].astype(F32)
            for h in range(heads)
        )

    incoming = lax.fori_loop(0, s, chain, first)
    rec = []
    for h in range(heads):
        o = local[h] + dot(lifted[h], incoming[h].astype(BF16), NT)
        rec.append(rms(o, rgain[...]))
    rec_hidden = jnp.concatenate(rec, axis=1).astype(BF16)

    width = nf.shape[2]
    pieces = o_send.shape[0]
    step = width // pieces

    def o_copy(i, j):
        cols = pl.ds(i * step, step)
        return pltpu.make_async_remote_copy(
            src_ref=pbuf.at[tp_peer(j), :, cols], dst_ref=rbuf.at[j, :, cols],
            send_sem=o_send.at[i, j], recv_sem=o_recv.at[i, j],
            device_id=(s, tp_peer(j)), device_id_type=MESH,
        )

    per = n // pieces
    for i in range(pieces):
        wa = goa[i * per : (i + 1) * per].reshape(step, goa.shape[2])
        wb = gor[i * per : (i + 1) * per].reshape(step, gor.shape[2])
        part = (dot(attn_hidden, wa, NT) + dot(rec_hidden, wb, NT)).astype(BF16)
        pbuf[:, :, i * step : (i + 1) * step] = part.reshape(nt, rows, step)
        for j in range(1, nt):
            o_copy(i, j).start()
    for i in range(pieces):
        cols = slice(i * step, (i + 1) * step)
        acc = pbuf[t, :, cols].astype(F32)
        for j in range(1, nt):
            o_copy(i, j).wait_recv()
            acc = acc + rbuf[j, :, cols].astype(F32)
        out[:, cols] = acc.astype(out.dtype)

    finish(one)
    finish(two)
    for j in range(1, nt):
        n_copy(j).wait_send()
        kt_copy(j).wait_send()
        for i in range(pieces):
            o_copy(i, j).wait_send()
    loop(1, n, lambda j: kv_copy(j).wait_send())

    def st_done(j):
        for copy in st_pair(j, s + j, s):
            copy.wait_send()

    loop(1, n - s, st_done)


def solution(mesh):
    n, nt = mesh.shape["sp"], mesh.shape["tp"]

    def body(
        tokens, input_norm_gain, paired_query_weight, shared_key_weight, shared_value_weight,
        recurrent_query_weight, forget_gate_weight, recurrent_value_weight,
        attention_output_weight, recurrent_output_weight, attention_head_gain,
        recurrent_head_gain, second_map_weight, forget_leak_rate, extra_log_decay,
        initial_recurrent_state,
    ):
        rows, width = tokens.shape
        heads = initial_recurrent_state.shape[0]
        weights = (
            paired_query_weight, forget_gate_weight, recurrent_value_weight,
            recurrent_query_weight, attention_output_weight, recurrent_output_weight,
        )
        half = n // 2
        pieces = 4
        vm = pl.BlockSpec(memory_space=pltpu.VMEM)
        sm = pl.BlockSpec(memory_space=pltpu.SMEM)
        dma = pltpu.SemaphoreType.DMA
        w = RECURRENT_WIDTH
        return pl.pallas_call(
            functools.partial(kernel, n, nt),
            out_shape=jax.ShapeDtypeStruct((rows, width), BF16),
            in_specs=[vm] * 12 + [sm] + [vm] * 3,
            out_specs=vm,
            scratch_shapes=[pltpu.VMEM((n,) + a.shape, BF16) for a in weights]
            + [
                pltpu.VMEM((nt, rows, width), BF16),
                pltpu.VMEM((nt, n, rows, 2 * QK_DIM + HEAD_DIM), BF16),
                pltpu.VMEM((n, heads, w, w), BF16),
                pltpu.VMEM((n, 8, heads * w), F32),
                pltpu.VMEM((nt, rows, width), BF16),
                pltpu.VMEM((nt, rows, width), BF16),
                dma((6, 2, half)), dma((6, 2, half)),
                dma((nt,)), dma((nt,)),
                dma((n,)), dma((n,)),
                dma((nt,)), dma((nt,)),
                dma((n,)), dma((n,)),
                dma((n,)), dma((n,)),
                dma((pieces, nt)), dma((pieces, nt)),
            ],
            compiler_params=pltpu.CompilerParams(
                has_side_effects=True, vmem_limit_bytes=60 * 1024 * 1024
            ),
        )(
            tokens, input_norm_gain[None], *weights, shared_key_weight, shared_value_weight,
            attention_head_gain[None], recurrent_head_gain[None], second_map_weight,
            forget_leak_rate[None], extra_log_decay, initial_recurrent_state,
        )

    placed = (
        P(("sp", "tp"), None), P(), P("sp", "tp"), P(), P(), P("sp", "tp"), P("sp", "tp"),
        P("sp", "tp"), P("sp", "tp"), P("sp", "tp"), P(), P(), P("tp"), P("tp"),
        P("sp", "tp"), P("tp", None, None),
    )
    return jax.shard_map(
        body, mesh=mesh, in_specs=placed, out_specs=P(("sp", "tp"), None), check_vma=False
    )
```

```python
import functools
import math

import jax
import jax.numpy as jnp
from jax import lax
from jax.experimental import pallas as pl
from jax.experimental.pallas import tpu as pltpu
from jax.sharding import PartitionSpec as P

QK_DIM = 32
HEAD_DIM = 64
RECURRENT_WIDTH = 128
REC_SPAN = 64
KEY_BLOCK = 1536
EPS = 1e-06
MESH = pl.DeviceIdType.MESH
F32, BF16 = jnp.float32, jnp.bfloat16

NN = (((1,), (0,)), ((), ()))
NT = (((1,), (1,)), ((), ()))
TN = (((0,), (0,)), ((), ()))


def dot(a, b, dims=NN, precision=None):
    return lax.dot_general(a, b, dims, preferred_element_type=F32, precision=precision)


def rms(x, gain):
    return x * lax.rsqrt(jnp.mean(x * x, axis=-1, keepdims=True) + EPS) * gain


def loop(lo, hi, body):
    def step(j, carry):
        body(j)
        return carry

    lax.fori_loop(lo, hi, step, 0)


def kernel(
    n, nt,
    tok, gain, wq, wg, wv, wr, woa, wor, wk, wval, again, rgain, mapw, leak, extra, init,
    out,
    gq, gg, gv, gr, goa, gor, nf, kv, pair, pair_d, units, units_d, prefix, pbuf, rbuf,
    ring_send, ring_recv, n_send, n_recv, kv_send, kv_recv, kt_send, kt_recv,
    p_send, p_recv, st_send, st_recv, de_send, de_recv, o_send, o_recv,
):
    s, t = lax.axis_index("sp"), lax.axis_index("tp")
    half = n // 2
    x, z = s % 2, s // 2
    pos = (1 - x) * z + x * (n - 1 - z)

    def at(p):
        p = (p + 2 * n) % n
        hi = p // half
        return (1 - hi) * 2 * p + hi * (2 * (n - 1 - p) + 1)

    ins = (wq, wg, wv, wr, woa, wor)
    bufs = (gq, gg, gv, gr, goa, gor)
    longer = (1, 0, 1, 0, 1, 1)

    def hops(a, d):
        return half if longer[a] == d else half - 1

    def send(a, d, k, first):
        sign = 1 - 2 * d
        owner = s if first else at(pos - sign * k)
        return pltpu.make_async_remote_copy(
            src_ref=ins[a] if first else bufs[a].at[owner],
            dst_ref=bufs[a].at[owner],
            send_sem=ring_send.at[a, d, k],
            recv_sem=ring_recv.at[a, d, k],
            device_id=(at(pos + sign), t),
            device_id_type=MESH,
        )

    def arrival(a, d, k):
        sign = 1 - 2 * d
        slot = bufs[a].at[at(pos - sign * (k + 1))]
        return pltpu.make_async_remote_copy(
            src_ref=slot, dst_ref=slot,
            send_sem=ring_send.at[a, d, k], recv_sem=ring_recv.at[a, d, k],
            device_id=(at(pos - sign), t), device_id_type=MESH,
        )

    def start(group):
        for a in group:
            for d in (0, 1):
                send(a, d, 0, True).start()

    def ring_hop(group, k):
        for a in group:
            for d in (0, 1):
                count = hops(a, d)

                @pl.when(k < count)
                def _():
                    arrival(a, d, k).wait_recv()

                @pl.when(k + 1 < count)
                def _():
                    send(a, d, k + 1, False).start()

    def ring(group, lo, hi):
        if n <= 8:
            for k in range(lo, hi):
                ring_hop(group, k)
        else:
            loop(lo, hi, lambda k: ring_hop(group, k))

    def finish(group):
        for a in group:
            for d in (0, 1):
                send(a, d, 0, True).wait_send()
                loop(1, hops(a, d), lambda k: send(a, d, k, False).wait_send())

    one, two, three = (1, 2), (3, 0), (4, 5)
    cut = [half * i // 4 for i in range(5)]
    barrier = pltpu.get_barrier_semaphore()

    def greet(peer):
        pl.semaphore_signal(barrier, inc=1, device_id=peer, device_id_type=MESH)

    loop(1, n, lambda j: greet(((s + j) % n, t)))
    for j in range(1, nt):
        greet((s, (t + j) % nt))
    pl.semaphore_wait(barrier, n + nt - 2)
    start(one)

    rows = tok.shape[0]
    normed = rms(tok[...].astype(F32), gain[...]).astype(BF16)
    nf[t] = normed

    def tp_peer(j):
        return (t + j) % nt

    def n_copy(j):
        return pltpu.make_async_remote_copy(
            src_ref=nf.at[t], dst_ref=nf.at[t], send_sem=n_send.at[j], recv_sem=n_recv.at[j],
            device_id=(s, tp_peer(j)), device_id_type=MESH,
        )

    def n_in(j):
        slot = nf.at[(t + nt - j) % nt]
        return pltpu.make_async_remote_copy(
            src_ref=slot, dst_ref=slot, send_sem=n_send.at[j], recv_sem=n_recv.at[j],
            device_id=(s, (t + nt - j) % nt), device_id_type=MESH,
        )

    kv[t, s] = jnp.concatenate(
        [dot(normed, wk[...], NT).astype(BF16), dot(normed, wval[...], NT).astype(BF16)], axis=1
    )
    for j in range(1, nt):
        n_copy(j).start()

    def kv_copy(j):
        return pltpu.make_async_remote_copy(
            src_ref=kv.at[t, s], dst_ref=kv.at[t, s],
            send_sem=kv_send.at[j], recv_sem=kv_recv.at[j],
            device_id=((s + j) % n, t), device_id_type=MESH,
        )

    def kv_in(j):
        slot = kv.at[t, (s + n - j) % n]
        return pltpu.make_async_remote_copy(
            src_ref=slot, dst_ref=slot, send_sem=kv_send.at[j], recv_sem=kv_recv.at[j],
            device_id=((s + n - j) % n, t), device_id_type=MESH,
        )

    def kt_copy(j):
        return pltpu.make_async_remote_copy(
            src_ref=kv.at[t], dst_ref=kv.at[t], send_sem=kt_send.at[j], recv_sem=kt_recv.at[j],
            device_id=(s, tp_peer(j)), device_id_type=MESH,
        )

    def kt_in(j):
        slot = kv.at[(t + nt - j) % nt]
        return pltpu.make_async_remote_copy(
            src_ref=slot, dst_ref=slot, send_sem=kt_send.at[j], recv_sem=kt_recv.at[j],
            device_id=(s, (t + nt - j) % nt), device_id_type=MESH,
        )

    loop(1, n, lambda j: kv_copy(j).start())
    for a in range(6):
        bufs[a][s] = ins[a][...]

    ring(one, 0, max(cut[1], 1))
    loop(1, n, lambda j: kv_in(j).wait_recv())
    for j in range(1, nt):
        kt_copy(j).start()
    ring(one, max(cut[1], 1), half - 1)
    start(two)
    for j in range(1, nt):
        n_in(j).wait_recv()
        kt_in(j).wait_recv()
    ring(one, half - 1, half)

    count = nt * rows
    full = nf[...].reshape(count, nf.shape[2])

    def project(buf):
        return dot(full, buf[...].reshape(full.shape[1], buf.shape[2])).astype(BF16)

    gate = project(gg).astype(F32)
    vals = project(gv)
    ring(two, cut[0], cut[1])

    inflow = leak[...] * (1.0 - jax.nn.sigmoid(gate))
    log_decay = jnp.log(1.0 - inflow) + extra[...]
    spans = count // REC_SPAN
    rr = lax.broadcasted_iota(jnp.int32, (REC_SPAN, REC_SPAN), 0)
    cc = lax.broadcasted_iota(jnp.int32, (REC_SPAN, REC_SPAN), 1)
    lower = (rr >= cc).astype(F32)
    running, offsets = [], []
    offset = jnp.zeros((1, log_decay.shape[1]), F32)
    for i in range(spans):
        part = log_decay[i * REC_SPAN : (i + 1) * REC_SPAN]
        run = dot(lower, part, precision=lax.Precision.HIGHEST)
        running.append(run)
        offsets.append(offset)
        offset = offset + run[REC_SPAN - 1 : REC_SPAN]
    total = offset
    w = RECURRENT_WIDTH
    heads = log_decay.shape[1] // w
    befores = [[None] * spans for _ in range(heads)]
    for h in range(heads):
        c = slice(h * w, (h + 1) * w)
        carried = None
        for i in range(spans):
            r = slice(i * REC_SPAN, (i + 1) * REC_SPAN)
            befores[h][i] = carried
            final = running[i][REC_SPAN - 1 : REC_SPAN, c]
            weight = (inflow[r, c] * jnp.exp(final - running[i][:, c])).astype(BF16)
            new = dot(vals[r, c], weight, TN)
            carried = new if carried is None else carried * jnp.exp(final) + new
        pair[x, h] = carried.astype(BF16)
        pair_d[x, h] = jnp.broadcast_to(total[:, c], pair_d.shape[2:])

    mate = s + 1 - 2 * x

    def mate_copy(i, ref):
        return pltpu.make_async_remote_copy(
            src_ref=ref, dst_ref=ref, send_sem=p_send.at[i], recv_sem=p_recv.at[i],
            device_id=(mate, t), device_id_type=MESH,
        )

    def st_pair(j, peer, owner):
        return (
            pltpu.make_async_remote_copy(
                src_ref=units.at[owner], dst_ref=units.at[owner],
                send_sem=st_send.at[j], recv_sem=st_recv.at[j],
                device_id=(2 * peer + x, t), device_id_type=MESH,
            ),
            pltpu.make_async_remote_copy(
                src_ref=units_d.at[owner], dst_ref=units_d.at[owner],
                send_sem=de_send.at[j], recv_sem=de_recv.at[j],
                device_id=(2 * peer + x, t), device_id_type=MESH,
            ),
        )

    def st_start(j):
        for copy in st_pair(j, z + j, z):
            copy.start()

    def st_wait(j):
        for copy in st_pair(j, z - j, z - j):
            copy.wait_recv()

    mate_copy(0, pair.at[x]).start()
    mate_copy(1, pair_d.at[x]).start()
    ring(two, cut[1], cut[2])
    mate_copy(0, pair.at[1 - x]).wait_recv()
    mate_copy(1, pair_d.at[1 - x]).wait_recv()
    units[z] = (
        pair[0, x].astype(F32) * jnp.exp(pair_d[1, x][0:1]) + pair[1, x].astype(F32)
    ).astype(BF16)
    units_d[z] = pair_d[0, x] + pair_d[1, x]
    loop(1, half - z, st_start)
    ring(two, cut[2], half - 1)
    start(three)
    ring(two, half - 1, half)
    queries = project(gq)
    raw = project(gr).astype(F32)

    key_total = kv.shape[0] * kv.shape[1] * kv.shape[2]
    owners = max(1, min(n, KEY_BLOCK // (nt * rows)))
    blocks = n // owners
    scale = 1.0 / math.sqrt(QK_DIM)

    def attend(h, b):
        both = kv[:, pl.ds(b * owners, owners)].reshape(nt * owners * rows, kv.shape[3])
        values = both[:, 2 * QK_DIM :]
        parts = []
        for comp in range(2):
            lo = (2 * h + comp) * QK_DIM
            keys = both[:, comp * QK_DIM : (comp + 1) * QK_DIM]
            scores = dot(queries[:, lo : lo + QK_DIM], keys, NT) * scale
            peak = jnp.max(scores, axis=1, keepdims=True)
            expo = jnp.exp(scores - peak)
            parts += [peak, jnp.sum(expo, axis=1, keepdims=True), dot(expo.astype(BF16), values)]
        return tuple(parts)

    def merge(a, b):
        parts = []
        for comp in range(2):
            pa, ta, wa = a[3 * comp : 3 * comp + 3]
            pb, tb, wb = b[3 * comp : 3 * comp + 3]
            peak = jnp.maximum(pa, pb)
            ea, eb = jnp.exp(pa - peak), jnp.exp(pb - peak)
            parts += [peak, ta * ea + tb * eb, wa * ea + wb * eb]
        return tuple(parts)

    attn_heads = queries.shape[1] // (2 * QK_DIM)
    hidden = []
    for h in range(attn_heads):
        got = attend(h, 0)
        if blocks > 1:
            got = lax.fori_loop(1, blocks, lambda b, g: merge(g, attend(h, b)), got)
        blended = got[2] / got[1] - mapw[h] * (got[5] / got[4])
        hidden.append(rms(blended, again[...]))
        if h == 0:
            ring(three, cut[0], cut[1])
            loop(1, z + 1, st_wait)

            def chain(k, carry):
                return carry * jnp.exp(units_d[k][0:1]) + units[k].astype(F32)

            prefix[x] = lax.fori_loop(0, z, chain, init[x].T).astype(BF16)
            mate_copy(2, prefix.at[x]).start()
    attn_hidden = jnp.concatenate(hidden, axis=1).astype(BF16)
    ring(three, cut[1], cut[2])

    rec_query = raw * jax.nn.sigmoid(raw)
    local, lifted = [], []
    for h in range(heads):
        c = slice(h * RECURRENT_WIDTH, (h + 1) * RECURRENT_WIDTH)
        outs, lifts = [], []
        for i in range(spans):
            r = slice(i * REC_SPAN, (i + 1) * REC_SPAN)
            run = running[i][:, c]
            dq = (rec_query[r, c] * jnp.exp(run)).astype(BF16)
            within = dot(dq, (inflow[r, c] * jnp.exp(-run)).astype(BF16), NT) * lower
            o = dot(within.astype(BF16), vals[r, c])
            if befores[h][i] is not None:
                o = o + dot(dq, befores[h][i].astype(BF16), NT)
            outs.append(o)
            lifts.append(rec_query[r, c] * jnp.exp(offsets[i][:, c] + run))
        local.append(jnp.concatenate(outs, axis=0))
        lifted.append(jnp.concatenate(lifts, axis=0).astype(BF16))

    mate_copy(2, prefix.at[1 - x]).wait_recv()
    rec = []
    for h in range(heads):
        base = prefix[h].astype(F32)
        later = base * jnp.exp(pair_d[0, h][0:1]) + pair[0, h].astype(F32)
        incoming = jnp.where(x == 1, later, base)
        o = local[h] + dot(lifted[h], incoming.astype(BF16), NT)
        rec.append(rms(o, rgain[...]))
    rec_hidden = jnp.concatenate(rec, axis=1).astype(BF16)

    part_width = pbuf.shape[3]

    def o_copy(b, j):
        return pltpu.make_async_remote_copy(
            src_ref=pbuf.at[b, tp_peer(j)], dst_ref=rbuf.at[b, j],
            send_sem=o_send.at[b, j], recv_sem=o_recv.at[b, j],
            device_id=(s, tp_peer(j)), device_id_type=MESH,
        )

    def out_block(b):
        part = dot(attn_hidden, goa[b], NT) + dot(rec_hidden, gor[b], NT)
        pbuf[b] = part.astype(BF16).reshape(nt, rows, part_width)
        for j in range(1, nt):
            o_copy(b, j).start()

    def both_sides(k):
        out_block(at(pos - k - 1))
        out_block(at(pos + k + 1))

    def repeat(lo, hi, body):
        if n <= 8:
            for k in range(lo, hi):
                body(k)
        else:
            loop(lo, hi, body)

    def arrive(k):
        ring_hop(three, k)
        both_sides(k)

    out_block(s)
    repeat(0, cut[2], both_sides)
    repeat(cut[2], half - 1, arrive)
    ring_hop(three, half - 1)
    out_block(at(pos + half))
    for b in range(n):
        acc = pbuf[b, t].astype(F32)
        for j in range(1, nt):
            o_copy(b, j).wait_recv()
            acc = acc + rbuf[b, j].astype(F32)
        out[:, b * part_width : (b + 1) * part_width] = acc.astype(out.dtype)

    finish(one)
    finish(two)
    finish(three)
    for j in range(1, nt):
        n_copy(j).wait_send()
        kt_copy(j).wait_send()
    loop(1, n, lambda j: kv_copy(j).wait_send())

    def st_done(j):
        for copy in st_pair(j, z + j, z):
            copy.wait_send()

    loop(1, half - z, st_done)
    mate_copy(0, pair.at[x]).wait_send()
    mate_copy(1, pair_d.at[x]).wait_send()
    mate_copy(2, prefix.at[x]).wait_send()

    def o_done(b):
        for j in range(1, nt):
            o_copy(b, j).wait_send()

    loop(0, n, o_done)


def solution(mesh):
    n, nt = mesh.shape["sp"], mesh.shape["tp"]

    def body(
        tokens, input_norm_gain, paired_query_weight, shared_key_weight, shared_value_weight,
        recurrent_query_weight, forget_gate_weight, recurrent_value_weight,
        attention_output_weight, recurrent_output_weight, attention_head_gain,
        recurrent_head_gain, second_map_weight, forget_leak_rate, extra_log_decay,
        initial_recurrent_state,
    ):
        rows, width = tokens.shape
        heads = initial_recurrent_state.shape[0]
        weights = (
            paired_query_weight, forget_gate_weight, recurrent_value_weight,
            recurrent_query_weight, attention_output_weight, recurrent_output_weight,
        )
        half = n // 2
        vm = pl.BlockSpec(memory_space=pltpu.VMEM)
        sm = pl.BlockSpec(memory_space=pltpu.SMEM)
        dma = pltpu.SemaphoreType.DMA
        w = RECURRENT_WIDTH
        return pl.pallas_call(
            functools.partial(kernel, n, nt),
            out_shape=jax.ShapeDtypeStruct((rows, width), BF16),
            in_specs=[vm] * 12 + [sm] + [vm] * 3,
            out_specs=vm,
            scratch_shapes=[pltpu.VMEM((n,) + a.shape, BF16) for a in weights]
            + [
                pltpu.VMEM((nt, rows, width), BF16),
                pltpu.VMEM((nt, n, rows, 2 * QK_DIM + HEAD_DIM), BF16),
                pltpu.VMEM((2, heads, w, w), BF16),
                pltpu.VMEM((2, heads, 8, w), F32),
                pltpu.VMEM((half, w, w), BF16),
                pltpu.VMEM((half, 8, w), F32),
                pltpu.VMEM((2, w, w), BF16),
                pltpu.VMEM((n, nt, rows, width // n), BF16),
                pltpu.VMEM((n, nt, rows, width // n), BF16),
                dma((6, 2, half)), dma((6, 2, half)),
                dma((nt,)), dma((nt,)),
                dma((n,)), dma((n,)),
                dma((nt,)), dma((nt,)),
                dma((3,)), dma((3,)),
                dma((half,)), dma((half,)),
                dma((half,)), dma((half,)),
                dma((n, nt)), dma((n, nt)),
            ],
            compiler_params=pltpu.CompilerParams(
                has_side_effects=True, collective_id=0, vmem_limit_bytes=60 * 1024 * 1024
            ),
        )(
            tokens, input_norm_gain[None], *weights, shared_key_weight.T, shared_value_weight.T,
            attention_head_gain[None], recurrent_head_gain[None], second_map_weight,
            forget_leak_rate[None], extra_log_decay, initial_recurrent_state,
        )

    placed = (
        P(("sp", "tp"), None), P(), P("sp", "tp"), P(), P(), P("sp", "tp"), P("sp", "tp"),
        P("sp", "tp"), P("sp", "tp"), P("sp", "tp"), P(), P(), P("tp"), P("tp"),
        P("sp", "tp"), P("tp", None, None),
    )
    return jax.shard_map(
        body, mesh=mesh, in_specs=placed, out_specs=P(("sp", "tp"), None), check_vma=False
    )
```

```python
import functools
import math

import jax
import jax.numpy as jnp
from jax import lax
from jax.experimental import pallas as pl
from jax.experimental.pallas import tpu as pltpu
from jax.sharding import PartitionSpec as P

QK_DIM = 32
HEAD_DIM = 64
RECURRENT_WIDTH = 128
REC_SPAN = 64
KEY_BLOCK = 1536
EPS = 1e-06
MESH = pl.DeviceIdType.MESH
F32, BF16 = jnp.float32, jnp.bfloat16

NN = (((1,), (0,)), ((), ()))
NT = (((1,), (1,)), ((), ()))
TN = (((0,), (0,)), ((), ()))


def dot(a, b, dims=NN, precision=None):
    return lax.dot_general(a, b, dims, preferred_element_type=F32, precision=precision)


def rms(x, gain):
    return x * lax.rsqrt(jnp.mean(x * x, axis=-1, keepdims=True) + EPS) * gain


def loop(lo, hi, body):
    def step(j, carry):
        body(j)
        return carry

    lax.fori_loop(lo, hi, step, 0)


def kernel(
    n, nt,
    tok, gain, wq, wg, wv, wr, woa, wor, wk, wval, again, rgain, mapw, leak, extra, init,
    out,
    gq, gg, gv, gr, goa, gor, nf, kv, pair, pair_d, units, units_d, prefix, pbuf, rbuf,
    ring_send, ring_recv, n_send, n_recv, kv_send, kv_recv, kt_send, kt_recv,
    p_send, p_recv, st_send, st_recv, de_send, de_recv, o_send, o_recv,
):
    s, t = lax.axis_index("sp"), lax.axis_index("tp")
    half = n // 2
    x, z = s % 2, s // 2
    pos = (1 - x) * z + x * (n - 1 - z)

    def at(p):
        p = (p + 2 * n) % n
        hi = p // half
        return (1 - hi) * 2 * p + hi * (2 * (n - 1 - p) + 1)

    ins = (wq, wg, wv, wr, woa, wor)
    bufs = (gq, gg, gv, gr, goa, gor)
    longer = (1, 0, 1, 0, 0, 1)

    def hops(a, d):
        return half if longer[a] == d else half - 1

    def send(a, d, k, first):
        sign = 1 - 2 * d
        owner = s if first else at(pos - sign * k)
        return pltpu.make_async_remote_copy(
            src_ref=ins[a] if first else bufs[a].at[owner],
            dst_ref=bufs[a].at[owner],
            send_sem=ring_send.at[a, d, k],
            recv_sem=ring_recv.at[a, d, k],
            device_id=(at(pos + sign), t),
            device_id_type=MESH,
        )

    def arrival(a, d, k):
        sign = 1 - 2 * d
        slot = bufs[a].at[at(pos - sign * (k + 1))]
        return pltpu.make_async_remote_copy(
            src_ref=slot, dst_ref=slot,
            send_sem=ring_send.at[a, d, k], recv_sem=ring_recv.at[a, d, k],
            device_id=(at(pos - sign), t), device_id_type=MESH,
        )

    def start(group):
        for a in group:
            for d in (0, 1):
                send(a, d, 0, True).start()

    def ring_hop(group, k):
        for a in group:
            for d in (0, 1):
                count = hops(a, d)

                @pl.when(k < count)
                def _():
                    arrival(a, d, k).wait_recv()

                @pl.when(k + 1 < count)
                def _():
                    send(a, d, k + 1, False).start()

    def ring(group, lo, hi):
        if n <= 8:
            for k in range(lo, hi):
                ring_hop(group, k)
        else:
            loop(lo, hi, lambda k: ring_hop(group, k))

    def finish(group):
        for a in group:
            for d in (0, 1):
                send(a, d, 0, True).wait_send()
                loop(1, hops(a, d), lambda k: send(a, d, k, False).wait_send())

    one, two, three = (1, 2), (3, 0), (4, 5)
    cut = [half * i // 4 for i in range(5)]
    barrier = pltpu.get_barrier_semaphore()

    def greet(peer):
        pl.semaphore_signal(barrier, inc=1, device_id=peer, device_id_type=MESH)

    loop(1, n, lambda j: greet(((s + j) % n, t)))
    for j in range(1, nt):
        greet((s, (t + j) % nt))
    pl.semaphore_wait(barrier, n + nt - 2)
    start(one)

    rows = tok.shape[0]
    normed = rms(tok[...].astype(F32), gain[...]).astype(BF16)
    nf[t] = normed

    def tp_peer(j):
        return (t + j) % nt

    def n_copy(j):
        return pltpu.make_async_remote_copy(
            src_ref=nf.at[t], dst_ref=nf.at[t], send_sem=n_send.at[j], recv_sem=n_recv.at[j],
            device_id=(s, tp_peer(j)), device_id_type=MESH,
        )

    def n_in(j):
        slot = nf.at[(t + nt - j) % nt]
        return pltpu.make_async_remote_copy(
            src_ref=slot, dst_ref=slot, send_sem=n_send.at[j], recv_sem=n_recv.at[j],
            device_id=(s, (t + nt - j) % nt), device_id_type=MESH,
        )

    kv[t, s] = jnp.concatenate(
        [dot(normed, wk[...], NT).astype(BF16), dot(normed, wval[...], NT).astype(BF16)], axis=1
    )
    for j in range(1, nt):
        n_copy(j).start()

    def kv_copy(j):
        return pltpu.make_async_remote_copy(
            src_ref=kv.at[t, s], dst_ref=kv.at[t, s],
            send_sem=kv_send.at[j], recv_sem=kv_recv.at[j],
            device_id=((s + j) % n, t), device_id_type=MESH,
        )

    def kv_in(j):
        slot = kv.at[t, (s + n - j) % n]
        return pltpu.make_async_remote_copy(
            src_ref=slot, dst_ref=slot, send_sem=kv_send.at[j], recv_sem=kv_recv.at[j],
            device_id=((s + n - j) % n, t), device_id_type=MESH,
        )

    def kt_copy(j):
        return pltpu.make_async_remote_copy(
            src_ref=kv.at[t], dst_ref=kv.at[t], send_sem=kt_send.at[j], recv_sem=kt_recv.at[j],
            device_id=(s, tp_peer(j)), device_id_type=MESH,
        )

    def kt_in(j):
        slot = kv.at[(t + nt - j) % nt]
        return pltpu.make_async_remote_copy(
            src_ref=slot, dst_ref=slot, send_sem=kt_send.at[j], recv_sem=kt_recv.at[j],
            device_id=(s, (t + nt - j) % nt), device_id_type=MESH,
        )

    loop(1, n, lambda j: kv_copy(j).start())
    for a in range(6):
        bufs[a][s] = ins[a][...]

    ring(one, 0, max(cut[1], 1))
    loop(1, n, lambda j: kv_in(j).wait_recv())
    for j in range(1, nt):
        kt_copy(j).start()
    ring(one, max(cut[1], 1), half - 1)
    start(two)
    for j in range(1, nt):
        n_in(j).wait_recv()
        kt_in(j).wait_recv()
    ring(one, half - 1, half)

    count = nt * rows
    full = nf[...].reshape(count, nf.shape[2])

    def project(buf):
        return dot(full, buf[...].reshape(full.shape[1], buf.shape[2])).astype(BF16)

    gate = project(gg).astype(F32)
    vals = project(gv)
    ring(two, cut[0], cut[1])

    inflow = leak[...] * (1.0 - jax.nn.sigmoid(gate))
    log_decay = jnp.log(1.0 - inflow) + extra[...]
    spans = count // REC_SPAN
    rr = lax.broadcasted_iota(jnp.int32, (REC_SPAN, REC_SPAN), 0)
    cc = lax.broadcasted_iota(jnp.int32, (REC_SPAN, REC_SPAN), 1)
    lower = (rr >= cc).astype(F32)
    running, offsets = [], []
    offset = jnp.zeros((1, log_decay.shape[1]), F32)
    for i in range(spans):
        part = log_decay[i * REC_SPAN : (i + 1) * REC_SPAN]
        run = dot(lower, part, precision=lax.Precision.HIGHEST)
        running.append(run)
        offsets.append(offset)
        offset = offset + run[REC_SPAN - 1 : REC_SPAN]
    total = offset
    w = RECURRENT_WIDTH
    heads = log_decay.shape[1] // w
    befores = [[None] * spans for _ in range(heads)]
    for h in range(heads):
        c = slice(h * w, (h + 1) * w)
        carried = None
        for i in range(spans):
            r = slice(i * REC_SPAN, (i + 1) * REC_SPAN)
            befores[h][i] = carried
            final = running[i][REC_SPAN - 1 : REC_SPAN, c]
            weight = (inflow[r, c] * jnp.exp(final - running[i][:, c])).astype(BF16)
            new = dot(vals[r, c], weight, TN)
            carried = new if carried is None else carried * jnp.exp(final) + new
        pair[x, h] = carried.astype(BF16)
        pair_d[x, h] = jnp.broadcast_to(total[:, c], pair_d.shape[2:])

    mate = s + 1 - 2 * x

    def mate_copy(i, ref):
        return pltpu.make_async_remote_copy(
            src_ref=ref, dst_ref=ref, send_sem=p_send.at[i], recv_sem=p_recv.at[i],
            device_id=(mate, t), device_id_type=MESH,
        )

    def st_pair(j, peer, owner):
        return (
            pltpu.make_async_remote_copy(
                src_ref=units.at[owner], dst_ref=units.at[owner],
                send_sem=st_send.at[j], recv_sem=st_recv.at[j],
                device_id=(2 * peer + x, t), device_id_type=MESH,
            ),
            pltpu.make_async_remote_copy(
                src_ref=units_d.at[owner], dst_ref=units_d.at[owner],
                send_sem=de_send.at[j], recv_sem=de_recv.at[j],
                device_id=(2 * peer + x, t), device_id_type=MESH,
            ),
        )

    def st_start(j):
        for copy in st_pair(j, z + j, z):
            copy.start()

    def st_wait(j):
        for copy in st_pair(j, z - j, z - j):
            copy.wait_recv()

    mate_copy(0, pair.at[x]).start()
    mate_copy(1, pair_d.at[x]).start()
    ring(two, cut[1], cut[2])
    mate_copy(0, pair.at[1 - x]).wait_recv()
    mate_copy(1, pair_d.at[1 - x]).wait_recv()
    units[z] = (
        pair[0, x].astype(F32) * jnp.exp(pair_d[1, x][0:1]) + pair[1, x].astype(F32)
    ).astype(BF16)
    units_d[z] = pair_d[0, x] + pair_d[1, x]
    loop(1, half - z, st_start)
    ring(two, cut[2], half - 1)
    start(three)
    ring(two, half - 1, half)
    queries = project(gq)
    raw = project(gr).astype(F32)

    key_total = kv.shape[0] * kv.shape[1] * kv.shape[2]
    owners = max(1, min(n, KEY_BLOCK // (nt * rows)))
    blocks = n // owners
    scale = 1.0 / math.sqrt(QK_DIM)

    def attend(h, b):
        both = kv[:, pl.ds(b * owners, owners)].reshape(nt * owners * rows, kv.shape[3])
        values = both[:, 2 * QK_DIM :]
        parts = []
        for comp in range(2):
            lo = (2 * h + comp) * QK_DIM
            keys = both[:, comp * QK_DIM : (comp + 1) * QK_DIM]
            scores = dot(queries[:, lo : lo + QK_DIM], keys, NT) * scale
            peak = jnp.max(scores, axis=1, keepdims=True)
            expo = jnp.exp(scores - peak)
            parts += [peak, jnp.sum(expo, axis=1, keepdims=True), dot(expo.astype(BF16), values)]
        return tuple(parts)

    def merge(a, b):
        parts = []
        for comp in range(2):
            pa, ta, wa = a[3 * comp : 3 * comp + 3]
            pb, tb, wb = b[3 * comp : 3 * comp + 3]
            peak = jnp.maximum(pa, pb)
            ea, eb = jnp.exp(pa - peak), jnp.exp(pb - peak)
            parts += [peak, ta * ea + tb * eb, wa * ea + wb * eb]
        return tuple(parts)

    attn_heads = queries.shape[1] // (2 * QK_DIM)
    hidden = []
    for h in range(attn_heads):
        got = attend(h, 0)
        if blocks > 1:
            got = lax.fori_loop(1, blocks, lambda b, g: merge(g, attend(h, b)), got)
        blended = got[2] / got[1] - mapw[h] * (got[5] / got[4])
        hidden.append(rms(blended, again[...]))
        if h == 0:
            ring(three, cut[0], cut[1])
            loop(1, z + 1, st_wait)

            def chain(k, carry):
                return carry * jnp.exp(units_d[k][0:1]) + units[k].astype(F32)

            prefix[x] = lax.fori_loop(0, z, chain, init[x].T).astype(BF16)
            mate_copy(2, prefix.at[x]).start()
    attn_hidden = jnp.concatenate(hidden, axis=1).astype(BF16)
    ring(three, cut[1], cut[2])

    rec_query = raw * jax.nn.sigmoid(raw)
    local, lifted = [], []
    for h in range(heads):
        c = slice(h * RECURRENT_WIDTH, (h + 1) * RECURRENT_WIDTH)
        outs, lifts = [], []
        for i in range(spans):
            r = slice(i * REC_SPAN, (i + 1) * REC_SPAN)
            run = running[i][:, c]
            dq = (rec_query[r, c] * jnp.exp(run)).astype(BF16)
            within = dot(dq, (inflow[r, c] * jnp.exp(-run)).astype(BF16), NT) * lower
            o = dot(within.astype(BF16), vals[r, c])
            if befores[h][i] is not None:
                o = o + dot(dq, befores[h][i].astype(BF16), NT)
            outs.append(o)
            lifts.append(rec_query[r, c] * jnp.exp(offsets[i][:, c] + run))
        local.append(jnp.concatenate(outs, axis=0))
        lifted.append(jnp.concatenate(lifts, axis=0).astype(BF16))

    mate_copy(2, prefix.at[1 - x]).wait_recv()
    rec = []
    for h in range(heads):
        base = prefix[h].astype(F32)
        later = base * jnp.exp(pair_d[0, h][0:1]) + pair[0, h].astype(F32)
        incoming = jnp.where(x == 1, later, base)
        o = local[h] + dot(lifted[h], incoming.astype(BF16), NT)
        rec.append(rms(o, rgain[...]))
    rec_hidden = jnp.concatenate(rec, axis=1).astype(BF16)

    part_width = pbuf.shape[3]

    def o_copy(b, j):
        return pltpu.make_async_remote_copy(
            src_ref=pbuf.at[b, tp_peer(j)], dst_ref=rbuf.at[b, j],
            send_sem=o_send.at[b, j], recv_sem=o_recv.at[b, j],
            device_id=(s, tp_peer(j)), device_id_type=MESH,
        )

    def out_block(b):
        part = dot(attn_hidden, goa[b], NT) + dot(rec_hidden, gor[b], NT)
        pbuf[b] = part.astype(BF16).reshape(nt, rows, part_width)
        for j in range(1, nt):
            o_copy(b, j).start()

    def both_sides(k):
        out_block(at(pos - k - 1))
        out_block(at(pos + k + 1))

    def repeat(lo, hi, body):
        if n <= 8:
            for k in range(lo, hi):
                body(k)
        else:
            loop(lo, hi, body)

    def arrive(k):
        ring_hop(three, k)
        both_sides(k)

    out_block(s)
    repeat(0, cut[2], both_sides)
    repeat(cut[2], half - 1, arrive)
    ring_hop(three, half - 1)
    out_block(at(pos + half))
    for b in range(n):
        acc = pbuf[b, t].astype(F32)
        for j in range(1, nt):
            o_copy(b, j).wait_recv()
            acc = acc + rbuf[b, j].astype(F32)
        out[:, b * part_width : (b + 1) * part_width] = acc.astype(out.dtype)

    finish(one)
    finish(two)
    finish(three)
    for j in range(1, nt):
        n_copy(j).wait_send()
        kt_copy(j).wait_send()
    loop(1, n, lambda j: kv_copy(j).wait_send())

    def st_done(j):
        for copy in st_pair(j, z + j, z):
            copy.wait_send()

    loop(1, half - z, st_done)
    mate_copy(0, pair.at[x]).wait_send()
    mate_copy(1, pair_d.at[x]).wait_send()
    mate_copy(2, prefix.at[x]).wait_send()

    def o_done(b):
        for j in range(1, nt):
            o_copy(b, j).wait_send()

    loop(0, n, o_done)


def solution(mesh):
    n, nt = mesh.shape["sp"], mesh.shape["tp"]

    def body(
        tokens, input_norm_gain, paired_query_weight, shared_key_weight, shared_value_weight,
        recurrent_query_weight, forget_gate_weight, recurrent_value_weight,
        attention_output_weight, recurrent_output_weight, attention_head_gain,
        recurrent_head_gain, second_map_weight, forget_leak_rate, extra_log_decay,
        initial_recurrent_state,
    ):
        rows, width = tokens.shape
        heads = initial_recurrent_state.shape[0]
        weights = (
            paired_query_weight, forget_gate_weight, recurrent_value_weight,
            recurrent_query_weight, attention_output_weight, recurrent_output_weight,
        )
        half = n // 2
        vm = pl.BlockSpec(memory_space=pltpu.VMEM)
        sm = pl.BlockSpec(memory_space=pltpu.SMEM)
        dma = pltpu.SemaphoreType.DMA
        w = RECURRENT_WIDTH
        return pl.pallas_call(
            functools.partial(kernel, n, nt),
            out_shape=jax.ShapeDtypeStruct((rows, width), BF16),
            in_specs=[vm] * 12 + [sm] + [vm] * 3,
            out_specs=vm,
            scratch_shapes=[pltpu.VMEM((n,) + a.shape, BF16) for a in weights]
            + [
                pltpu.VMEM((nt, rows, width), BF16),
                pltpu.VMEM((nt, n, rows, 2 * QK_DIM + HEAD_DIM), BF16),
                pltpu.VMEM((2, heads, w, w), BF16),
                pltpu.VMEM((2, heads, 8, w), F32),
                pltpu.VMEM((half, w, w), BF16),
                pltpu.VMEM((half, 8, w), F32),
                pltpu.VMEM((2, w, w), BF16),
                pltpu.VMEM((n, nt, rows, width // n), BF16),
                pltpu.VMEM((n, nt, rows, width // n), BF16),
                dma((6, 2, half)), dma((6, 2, half)),
                dma((nt,)), dma((nt,)),
                dma((n,)), dma((n,)),
                dma((nt,)), dma((nt,)),
                dma((3,)), dma((3,)),
                dma((half,)), dma((half,)),
                dma((half,)), dma((half,)),
                dma((n, nt)), dma((n, nt)),
            ],
            compiler_params=pltpu.CompilerParams(
                has_side_effects=True, collective_id=0, vmem_limit_bytes=60 * 1024 * 1024
            ),
        )(
            tokens, input_norm_gain[None], *weights, shared_key_weight.T, shared_value_weight.T,
            attention_head_gain[None], recurrent_head_gain[None], second_map_weight,
            forget_leak_rate[None], extra_log_decay, initial_recurrent_state,
        )

    placed = (
        P(("sp", "tp"), None), P(), P("sp", "tp"), P(), P(), P("sp", "tp"), P("sp", "tp"),
        P("sp", "tp"), P("sp", "tp"), P("sp", "tp"), P(), P(), P("tp"), P("tp"),
        P("sp", "tp"), P("tp", None, None),
    )
    return jax.shard_map(
        body, mesh=mesh, in_specs=placed, out_specs=P(("sp", "tp"), None), check_vma=False
    )
```
